256 devices in a mesh: sp: 32 (over z, x), tp: 4 (over y), dp: 2 (over core).
Axes of the slice: x: 4, y: 4, z: 8, core: 2. Of those that a mesh axis runs over, the one named last changes fastest.
Arguments:
- latent: bfloat16 [2, 16384, 2048], P('dp', ('sp', 'tp')), may hold values from -6 to 6
- condition: float32 [2, 2048], P('dp'), may hold values from -6 to 6
- context: bfloat16 [2, 1024, 2048], P('dp', 'sp'), may hold values from -6 to 6
- context_cond: float32 [2048], replicated, may hold values from -6 to 6
- shift_matrix: bfloat16 [2048, 2048], P(('sp', 'tp')), may hold values from -0.125 to 0.125
- scale_matrix: bfloat16 [2048, 2048], P(('sp', 'tp')), may hold values from -0.125 to 0.125
- gate_matrix: bfloat16 [2048, 2048], P(('sp', 'tp')), may hold values from -0.125 to 0.125
- value_proj: bfloat16 [2048, 2048], P(None, 'tp'), may hold values from -0.125 to 0.125
- gate_proj: bfloat16 [2048, 2048], P(None, 'tp'), may hold values from -0.125 to 0.125
- write_proj: bfloat16 [2048, 1024], P(None, 'tp'), may hold values from -0.125 to 0.125
- read_proj: bfloat16 [2048, 1024], P(None, 'tp'), may hold values from -0.125 to 0.125
- step_proj: bfloat16 [2048, 2, 32], replicated, may hold values from -0.125 to 0.125
- decay_rate: float32 [2, 32], replicated, may hold values from 3.0456543e-05 to 0.0601
- pacing: float32 [2, 16384], P('dp'), may hold values from 0.2 to 4.3
- value_taps: float32 [5, 2048], replicated, may hold values from -2.5 to 2.5
- write_taps: float32 [5, 1024], replicated, may hold values from -2.5 to 2.5
- read_taps: float32 [5, 1024], replicated, may hold values from -2.5 to 2.5
- norm_gain: float32 [2048], replicated, may hold values from 0.1 to 1.9
- out_proj: bfloat16 [2048, 2048], P('tp'), may hold values from -0.125 to 0.125
Outputs:
- updated: bfloat16 [2, 16384, 2048], P('dp', ('sp', 'tp'))
The draws below stay inside these ranges and needn't reach their ends.
All inputs are finite; a program needn't handle non-finite values.
Results may differ from the reference program's by a relative error of at most 0.006.
Values may be sent and summed in bfloat16 or wider, within the bound.
No kernel may reach another device: no remote copies, remote signals or barrier semaphores. Data moves between devices by JAX's collectives and lax.ppermute only.
A program may use at most 128 MiB of HBM per device.

```python
import math
import jax
import jax.numpy as jnp
from jax import lax

D = 2048
WIDTH = 2048
HEAD = 64
GROUPS = 8
STATE = 128
CONV = 5
ROW = 64
BLOCK = 128
TOK_DEV = 512
CTX = 1024
SAMPLES = 2
TOKENS = 16384
HEADS = 32
CHANNEL_BLOCK = 512


def draw_latent(key, part):
    noise_key, scale_key, direction_key, strength_key = jax.random.split(key, 4)
    span_rows = TOK_DEV // 2
    span_count = TOKENS // span_rows
    noise = jax.random.normal(noise_key, (SAMPLES, TOKENS, D), jnp.float32)
    directions = jax.random.normal(direction_key, (SAMPLES, span_count, D), jnp.float32)
    strength = jax.random.uniform(strength_key, (SAMPLES, span_count, 1), jnp.float32, 1.0, 2.0)
    offsets = jnp.repeat(directions * strength, span_rows, axis=1)
    return jnp.clip(noise + offsets, -6.0, 6.0).astype(jnp.bfloat16)


def draw_decay_rate(key, part):
    pick_key, slow_key, quick_key = jax.random.split(key, 3)
    quick_mask = jax.random.randint(pick_key, (2, HEADS), 0, 2) == 0
    slow_rate = jnp.exp(jax.random.uniform(slow_key, (2, HEADS), jnp.float32, math.log(0.5), math.log(2.0))) / TOKENS
    quick_rate = jnp.exp(jax.random.uniform(quick_key, (2, HEADS), jnp.float32, math.log(0.02), math.log(0.06)))
    return jnp.where(quick_mask, quick_rate, slow_rate).astype(jnp.float32)


def draw_pacing(key, part):
    span_key, token_key = jax.random.split(key)
    span_rows = TOK_DEV // 2
    span_count = TOKENS // span_rows
    span_factor = jnp.exp(jax.random.uniform(span_key, (SAMPLES, span_count), jnp.float32, math.log(0.35), math.log(2.8)))
    token_factor = jax.random.uniform(token_key, (SAMPLES, TOKENS), jnp.float32, 0.6, 1.5)
    return (jnp.repeat(span_factor, span_rows, axis=1) * token_factor).astype(jnp.float32)


def block_levels(stream_key, dims, cuts, least, high):
    factor_of, own = 1.0, jax.random.fold_in(stream_key, 6)
    for axis_at, blocks in cuts:
        draws = jnp.exp(jax.random.uniform(jax.random.fold_in(own, axis_at), (blocks,), jnp.float32, least / len(cuts), high / len(cuts)))
        factor_of = factor_of * jnp.repeat(draws, dims[axis_at] // blocks).reshape([-1 if axis == axis_at else 1 for axis in range(len(dims))])
    return factor_of


def gaussian(stream_key, dims, scale, limit, cuts=(), kind=jnp.bfloat16):
    level = block_levels(stream_key, dims, cuts, -0.22, 0.18) if cuts else 1.0
    entries = jax.random.normal(stream_key, dims, jnp.float32) * scale * level
    return jnp.minimum(jnp.maximum(entries, -limit), limit).astype(kind)


def setup_inputs(seed: int = 0) -> dict:
    key_list = jax.random.split(jax.random.key(seed), 20)
    return {
        "latent": draw_latent(jax.random.fold_in(key_list[19], 71), 0),
        "condition": gaussian(key_list[1], (SAMPLES, D), 1.0, 6.0, ((0, 2),), jnp.float32),
        "context": gaussian(key_list[2], (SAMPLES, CTX, D), 1.0, 6.0, ((0, 2), (1, 32))),
        "context_cond": gaussian(key_list[3], (D,), 1.0, 6.0, (), jnp.float32),
        "shift_matrix": gaussian(key_list[4], (D, D), D ** -0.5, 0.125, ((0, 128),)),
        "scale_matrix": gaussian(key_list[5], (D, D), D ** -0.5, 0.125, ((0, 128),)),
        "gate_matrix": gaussian(key_list[6], (D, D), D ** -0.5, 0.125, ((0, 128),)),
        "value_proj": gaussian(key_list[7], (D, WIDTH), D ** -0.5, 0.125, ((1, 4),)),
        "gate_proj": gaussian(key_list[8], (D, WIDTH), D ** -0.5, 0.125, ((1, 4),)),
        "write_proj": gaussian(key_list[9], (D, GROUPS * STATE), D ** -0.5, 0.125, ((1, 4),)),
        "read_proj": gaussian(key_list[10], (D, GROUPS * STATE), D ** -0.5, 0.125, ((1, 4),)),
        "step_proj": gaussian(key_list[11], (D, 2, HEADS), D ** -0.5, 0.125),
        "decay_rate": draw_decay_rate(jax.random.fold_in(key_list[19], 71), 0),
        "pacing": draw_pacing(jax.random.fold_in(key_list[19], 71), 0),
        "value_taps": gaussian(key_list[14], (CONV, WIDTH), CONV ** -0.5, 2.5, (), jnp.float32),
        "write_taps": gaussian(key_list[15], (CONV, GROUPS * STATE), CONV ** -0.5, 2.5, (), jnp.float32),
        "read_taps": gaussian(key_list[16], (CONV, GROUPS * STATE), CONV ** -0.5, 2.5, (), jnp.float32),
        "norm_gain": jnp.clip(1.0 + 0.18 * jax.random.normal(key_list[17], (WIDTH,), jnp.float32), 0.1, 1.9),
        "out_proj": gaussian(key_list[18], (WIDTH, D), WIDTH ** -0.5, 0.125, ((0, 4),)),
    }


NORM_FLOOR = 1e-05
GATED_FLOOR = 1e-06
FINEST = lax.Precision.HIGHEST

def masked_exp(exponent, allowed):
    return jnp.where(allowed, jnp.exp(jnp.where(allowed, exponent, 0.0)), 0.0)

def modulate(row_block, shift_row, scale_row):
    values = row_block.astype(jnp.float32)
    center = lax.optimization_barrier(jnp.mean(values, -1, keepdims=True))
    spread = lax.optimization_barrier(jnp.mean(jnp.square(values - center), -1, keepdims=True))
    normed = (values - center) * lax.rsqrt(spread + NORM_FLOOR)
    return (normed * (1.0 + shift_row * 0.0 + scale_row) + shift_row).astype(jnp.bfloat16)

def convolve(values, kernel, run_count):
    length, channels = values.shape
    tap_count = kernel.shape[0]
    margin = tap_count // 2
    stretch = length // run_count
    blocked = values.astype(jnp.float32).reshape(run_count, stretch, channels)
    padded = jnp.pad(blocked, ((0, 0), (margin, margin), (0, 0)))
    summed = jnp.zeros_like(blocked)
    for offset in range(tap_count):
        summed = summed + padded[:, offset:offset + stretch] * kernel[offset]
    return jax.nn.silu(summed).reshape(length, channels).astype(jnp.bfloat16)

def context_state(values, writes, weight, groups):
    length = values.shape[0]
    per_group = weight.shape[1] // groups
    scaled = (writes.reshape(length, groups, 1, STATE) * weight.reshape(length, groups, per_group, 1)).astype(jnp.bfloat16)
    head_values = values.reshape(length, groups, per_group, HEAD)
    return jnp.einsum('lgrn,lgrp->grnp', scaled.astype(jnp.float32), head_values.astype(jnp.float32))

def block_sweep(values, writes, reads, decays, steps, start):
    length = values.shape[0]
    groups = writes.shape[1] // STATE
    per_group = decays.shape[1] // groups
    blocks = length // BLOCK
    head_values = values.reshape(blocks, BLOCK, groups, per_group, HEAD).astype(jnp.float32)
    write_rows = writes.reshape(blocks, BLOCK, groups, STATE)
    read_rows = reads.reshape(blocks, BLOCK, groups, STATE).astype(jnp.float32)
    cumulative = jnp.cumsum(decays.reshape(blocks, BLOCK, groups, per_group), axis=1)
    step_rows = steps.reshape(blocks, BLOCK, groups, per_group)
    lower_mask = jnp.tril(jnp.ones((BLOCK, BLOCK), bool))[:, :, None, None]

    def advance(carry_state, inputs):
        block_values, block_writes, block_reads, block_cumul, block_steps = inputs
        affinity = jnp.einsum('tgn,sgn->tsg', block_reads, block_writes.astype(jnp.float32))
        exponent = block_cumul[:, None] - block_cumul[None, :]
        mixing = (affinity[..., None] * masked_exp(exponent, lower_mask) * block_steps[None]).astype(jnp.bfloat16)
        within = jnp.einsum('tsgr,sgrp->tgrp', mixing.astype(jnp.float32), block_values)
        carried = jnp.einsum('tgn,grnp->tgrp', block_reads, carry_state, precision=FINEST) * jnp.exp(block_cumul)[..., None]
        weight = jnp.exp(block_cumul[-1:] - block_cumul) * block_steps
        scaled = (block_writes[:, :, None, :] * weight[..., None]).astype(jnp.bfloat16)
        increment = jnp.einsum('sgrn,sgrp->grnp', scaled.astype(jnp.float32), block_values)
        carry_state = jnp.exp(block_cumul[-1])[..., None, None] * carry_state + increment
        return (carry_state, within + carried)
    final_state, outputs = lax.scan(advance, start, (head_values, write_rows, read_rows, cumulative, step_rows))
    return outputs.reshape(length, groups * per_group * HEAD)

def reference(latent, condition, context, context_cond, shift_matrix, scale_matrix, gate_matrix, value_proj, gate_proj, write_proj, read_proj, step_proj, decay_rate, pacing, value_taps, write_taps, read_taps, norm_gain, out_proj):
    model_width = latent.shape[2]
    results = []
    for sample in range(latent.shape[0]):
        activated = jax.nn.silu(jnp.stack([condition[sample], context_cond])).astype(jnp.bfloat16)
        shifts = jnp.dot(activated, shift_matrix, preferred_element_type=jnp.float32)
        scales = jnp.dot(activated, scale_matrix, preferred_element_type=jnp.float32)
        gate_row = jnp.dot(activated[:1], gate_matrix, preferred_element_type=jnp.float32)
        hidden = modulate(latent[sample], shifts[0], scales[0])
        run_count = TOKENS // ROW
        values = convolve(jnp.dot(hidden, value_proj, preferred_element_type=jnp.float32).astype(jnp.bfloat16), value_taps, run_count)
        writes = convolve(jnp.dot(hidden, write_proj, preferred_element_type=jnp.float32).astype(jnp.bfloat16), write_taps, run_count)
        read_rows = convolve(jnp.dot(hidden, read_proj, preferred_element_type=jnp.float32).astype(jnp.bfloat16), read_taps, run_count)
        gate_pre = jnp.dot(hidden, gate_proj, preferred_element_type=jnp.float32).astype(jnp.bfloat16)
        step_raw = jnp.dot(hidden, step_proj.reshape(model_width, 2 * HEADS), preferred_element_type=jnp.float32).astype(jnp.bfloat16)
        step_raw = lax.optimization_barrier(step_raw).astype(jnp.float32).reshape(TOKENS, 2, HEADS)
        context_hidden = modulate(context[sample], shifts[1], scales[1])
        ctx_values = convolve(jnp.dot(context_hidden, value_proj, preferred_element_type=jnp.float32).astype(jnp.bfloat16), value_taps, 1)
        ctx_writes = convolve(jnp.dot(context_hidden, write_proj, preferred_element_type=jnp.float32).astype(jnp.bfloat16), write_taps, 1)
        ctx_raw = jnp.dot(context_hidden, step_proj.reshape(model_width, 2 * HEADS), preferred_element_type=jnp.float32).astype(jnp.bfloat16)
        ctx_raw = lax.optimization_barrier(ctx_raw).astype(jnp.float32).reshape(CTX, 2, HEADS)
        ctx_fwd_step = jax.nn.softplus(ctx_raw[:, 0])
        ctx_fwd_decay = -decay_rate[0][None, :] * ctx_fwd_step
        ctx_cumul = jnp.cumsum(ctx_fwd_decay, axis=0)
        ctx_forward = context_state(ctx_values, ctx_writes, jnp.exp(ctx_cumul[-1:] - ctx_cumul) * ctx_fwd_step, GROUPS)
        ctx_bwd_step = jax.nn.softplus(ctx_raw[:, 1])
        ctx_bwd_decay = -decay_rate[1][None, :] * ctx_bwd_step
        ctx_back_cumul = jnp.cumsum(ctx_bwd_decay, axis=0)
        ctx_backward = context_state(ctx_values, ctx_writes, jnp.exp(ctx_back_cumul - ctx_bwd_decay) * ctx_bwd_step, GROUPS)
        forward_step = jax.nn.softplus(step_raw[:, 0]) * pacing[sample][:, None]
        forward_decay = -decay_rate[0][None, :] * forward_step
        backward_step = jax.nn.softplus(step_raw[:, 1]) * pacing[sample][:, None]
        backward_decay = -decay_rate[1][None, :] * backward_step
        forward_out = block_sweep(values, writes, read_rows, forward_decay, forward_step, ctx_forward)
        backward_out = block_sweep(values[::-1], writes[::-1], read_rows[::-1], backward_decay[::-1], backward_step[::-1], ctx_backward)[::-1]
        gated_heads = (forward_out + backward_out) * jax.nn.silu(gate_pre.astype(jnp.float32))
        grouped = gated_heads.reshape(TOKENS, GROUPS, -1)
        grouped = grouped * lax.rsqrt(lax.optimization_barrier(jnp.mean(grouped * grouped, -1, keepdims=True)) + GATED_FLOOR)
        inner_rows = (grouped.reshape(TOKENS, WIDTH) * norm_gain).astype(jnp.bfloat16)
        summed = jnp.zeros((TOKENS, model_width), jnp.float32)
        for column_block in range(WIDTH // CHANNEL_BLOCK):
            lower_edge = column_block * CHANNEL_BLOCK
            portion = jnp.dot(inner_rows[:, lower_edge:lower_edge + CHANNEL_BLOCK], out_proj[lower_edge:lower_edge + CHANNEL_BLOCK], preferred_element_type=jnp.float32).astype(jnp.bfloat16)
            summed = summed + lax.optimization_barrier(portion).astype(jnp.float32)
        mixed = lax.optimization_barrier(summed.astype(jnp.bfloat16))
        results.append((latent[sample].astype(jnp.float32) + gate_row[0] * mixed.astype(jnp.float32)).astype(jnp.bfloat16))
    return jnp.stack(results)
```

```python
import jax
import jax.numpy as jnp
from jax import lax
from jax.experimental import pallas as pl
from jax.experimental.pallas import tpu as pltpu
from jax.sharding import Mesh
from jax.sharding import PartitionSpec as P

HEAD = 64
STATE = 128
ROW = 64
BLOCK = 128
TAPS = 5
NZ, NX, NY = 8, 4, 4
SP = ("sp_0", "sp_1")
SP_TP = ("sp_0", "sp_1", "tp")
NORM_FLOOR = 1e-05
GATED_FLOOR = 1e-06

D = 2048
ROWS = 128
TOK = NY * ROWS
BLOCKS = TOK // BLOCK
WD = 512
KD = 256
HEADS_DEV = 8
GROUPS_DEV = 2
CTX_DEV = 32
CTX_ROWS = CTX_DEV + 16
MSG = 2 * STATE + 16
ZMSG = STATE + 16

F32 = jnp.float32
BF16 = jnp.bfloat16


def iota(shape, dim):
    return lax.broadcasted_iota(jnp.int32, shape, dim)


def silu(v):
    return v / (1.0 + jnp.exp(-v))


def rounded(v):
    return v.astype(BF16).astype(F32)


def dot_f32(a, b):
    return jnp.dot(a, b, preferred_element_type=F32)


def dot_exact(a, b):
    return jnp.dot(a, b, precision=lax.Precision.HIGHEST, preferred_element_type=F32)


def dot_tn(a, b):
    return lax.dot_general(a, b, (((0,), (0,)), ((), ())), preferred_element_type=F32)


def dot_nt(a, b):
    return lax.dot_general(a, b, (((1,), (1,)), ((), ())), preferred_element_type=F32)


def mod_row(mod_ref, r):
    return jnp.concatenate([mod_ref[r * 16 + j : r * 16 + j + 1, :] for j in range(16)], axis=1)


def modulate(values, shift_row, scale_row):
    center = jnp.mean(values, -1, keepdims=True)
    spread = jnp.mean(jnp.square(values - center), -1, keepdims=True)
    normed = (values - center) * lax.rsqrt(spread + NORM_FLOOR)
    return (normed * (1.0 + scale_row) + shift_row).astype(BF16)


def head_lanes(cols, base):
    rows = cols.shape[0]
    low = iota((rows, 128), 1) < HEAD
    return jnp.concatenate(
        [
            jnp.where(
                low, cols[:, base + 2 * p : base + 2 * p + 1], cols[:, base + 2 * p + 1 : base + 2 * p + 2]
            )
            for p in range(HEADS_DEV // 2)
        ],
        axis=1,
    )


def head_row(column):
    own = iota((HEADS_DEV, WD), 1) // HEAD == iota((HEADS_DEV, WD), 0)
    return jnp.sum(jnp.where(own, column, 0.0), axis=0, keepdims=True)


def split_rows(row_f, row_b=None):
    out = jnp.zeros((16, 128), F32)
    at = iota((16, 128), 0)
    for start, row in ((0, row_f), (3, row_b)):
        if row is None:
            continue
        high = rounded(row)
        middle = rounded(row - high)
        low = (row - high) - middle
        for k, part in enumerate((high, middle, low)):
            out = jnp.where(at == start + k, part, out)
    return out.astype(BF16)


def joined_row(msg_ref, first):
    rows = msg_ref[first : first + 16, :].astype(F32)
    return (rows[0:1] + rows[1:2] + rows[2:3], rows[3:4] + rows[4:5] + rows[5:6])


def pack_states(scr, forward, backward, forward_decay, backward_decay):
    for q in range(NX):
        at = slice(q * 128, (q + 1) * 128)
        scr[q, 0:STATE, :] = forward[:, at].astype(BF16)
        scr[q, STATE : 2 * STATE, :] = backward[:, at].astype(BF16)
        scr[q, 2 * STATE :, :] = split_rows(forward_decay[:, at], backward_decay[:, at])


def send_order(scr, outs):
    x = lax.axis_index("sp_1")
    for d, out in enumerate(outs):
        out[...] = scr[lax.rem(x + d, NX)]


def call(body, outs, args, scratch=(), flops=1000000, name=None):
    vmem = pl.BlockSpec(memory_space=pltpu.VMEM)
    return pl.pallas_call(
        body,
        out_shape=tuple(jax.ShapeDtypeStruct(s, t) for s, t in outs),
        in_specs=[vmem] * len(args),
        out_specs=tuple(vmem for _ in outs),
        scratch_shapes=scratch,
        compiler_params=pltpu.CompilerParams(vmem_limit_bytes=48 * 1024 * 1024),
        cost_estimate=pl.CostEstimate(flops=flops, transcendentals=0, bytes_accessed=1000000),
        name=name,
    )(*args)


def mod_body(cond_ref, cctx_ref, sh_ref, sc_ref, ga_ref, o_ref):
    at = (lax.axis_index("sp_0") * NX + lax.axis_index("sp_1")) * NY + lax.axis_index("tp")
    base = pl.multiple_of((at // 8) * 128, 128)
    row = iota((8, 128), 0)
    lane = iota((8, 128), 1)
    both = jnp.where(
        row == 0, cond_ref[:, pl.ds(base, 128)], jnp.where(row == 1, cctx_ref[:, pl.ds(base, 128)], 0.0)
    )
    act = jnp.where(lane // 16 == lax.rem(at, 8), silu(both), 0.0).astype(BF16)
    for ref, first, count in ((sh_ref, 0, 2), (sc_ref, 2, 2), (ga_ref, 4, 1)):
        own = ref[...]
        res = dot_f32(act, jnp.concatenate([own] * 8, axis=0))
        for r in range(count):
            for j in range(16):
                to = (first + r) * 16 + j
                o_ref[to : to + 1, :] = res[r : r + 1, j * 128 : (j + 1) * 128]


def ctx_body(
    ctx_ref, left_ref, right_ref, mod_ref, wv_ref, ww_ref, ws_ref, rate_ref, vt_ref, wt_ref, o0, o1, o2, o3, scr
):
    sp = lax.axis_index("sp_0") * NX + lax.axis_index("sp_1")
    y = lax.axis_index("tp")
    raw_rows = jnp.concatenate(
        [left_ref[...].astype(F32), ctx_ref[...].astype(F32), right_ref[...].astype(F32)], axis=0
    )
    hidden = modulate(raw_rows, mod_row(mod_ref, 1), mod_row(mod_ref, 3))
    pre = jnp.concatenate(
        [dot_f32(hidden, wv_ref[...]).astype(BF16), dot_f32(hidden, ww_ref[...]).astype(BF16)], axis=1
    ).astype(F32)
    at = iota((CTX_ROWS, WD + KD), 0)
    inside = (at >= jnp.where(sp > 0, 0, 8)) & (at < jnp.where(sp < NZ * NX - 1, CTX_ROWS, CTX_DEV + 8))
    pre = jnp.where(inside, pre, 0.0).astype(BF16)
    raw = rounded(dot_f32(hidden, ws_ref[...])[8 : 8 + CTX_DEV])
    vcol = pl.multiple_of(y * WD, 128)
    wcol = pl.multiple_of(y * KD, 128)
    conv = jnp.zeros((CTX_DEV, WD + KD), F32)
    to_row = iota((CTX_DEV, CTX_ROWS), 0)
    from_row = iota((CTX_DEV, CTX_ROWS), 1)
    for k in range(TAPS):
        shift = (from_row == to_row + 6 + k).astype(BF16)
        taps = jnp.concatenate([vt_ref[k : k + 1, pl.ds(vcol, WD)], wt_ref[k : k + 1, pl.ds(wcol, KD)]], axis=1)
        conv = conv + dot_f32(shift, pre) * taps
    act = rounded(silu(conv))
    values = act[:, :WD]
    writes = act[:, WD:].astype(BF16)
    lane = iota((CTX_DEV, 128), 1)
    step = jax.nn.softplus(raw)
    decay = -rate_ref[0:1, :] * step
    lower = (iota((CTX_DEV, CTX_DEV), 1) <= iota((CTX_DEV, CTX_DEV), 0)).astype(F32)
    through = dot_exact(lower, decay)
    total = through[CTX_DEV - 1 :, :]
    weight = jnp.exp(jnp.where(lane < HEADS_DEV, total - through, through - decay)) * step
    scaled = [(values * head_lanes(weight, base)).astype(BF16) for base in (0, HEADS_DEV)]
    states = [
        jnp.concatenate(
            [dot_tn(writes[:, g * STATE : (g + 1) * STATE], s[:, g * 256 : (g + 1) * 256]) for g in range(GROUPS_DEV)],
            axis=1,
        )
        for s in scaled
    ]
    pack_states(scr, states[0], states[1], head_lanes(total, 0), head_lanes(total, HEADS_DEV))
    send_order(scr, (o0, o1, o2, o3))


def block_shifts():
    out = []
    for k in (0, 1, 3, 4):
        to_row = iota((BLOCK, BLOCK), 0)
        from_row = iota((BLOCK, BLOCK), 1)
        out.append(((from_row == to_row + (k - 2)) & (from_row // ROW == to_row // ROW)).astype(BF16))
    return jnp.concatenate(out, axis=0)


def convolved(pre, shifts, taps):
    moved = dot_f32(shifts, pre)
    total = moved[0:128] * taps[0:1]
    total = total + moved[128:256] * taps[1:2]
    total = total + pre.astype(F32) * taps[2:3]
    total = total + moved[256:384] * taps[3:4]
    total = total + moved[384:512] * taps[4:5]
    return silu(total).astype(BF16)


def first_body(
    own_ref,
    m1_ref,
    m2_ref,
    m3_ref,
    mod_ref,
    wv_ref,
    ww_ref,
    ws_ref,
    rate_ref,
    pace_ref,
    vt_ref,
    wt_ref,
    hid_ref,
    val_ref,
    wri_ref,
    aux_ref,
    col_ref,
    dec_ref,
    o0,
    o1,
    o2,
    o3,
    pre_ref,
    svf_ref,
    svb_ref,
    scr,
):
    sp = lax.axis_index("sp_0") * NX + lax.axis_index("sp_1")
    y = lax.axis_index("tp")
    shift_row = mod_row(mod_ref, 0)
    scale_row = mod_row(mod_ref, 2)
    for d, ref in enumerate((own_ref, m1_ref, m2_ref, m3_ref)):
        base = lax.rem(y - d + NY, NY) * ROWS

        def rows_at(i, carry, ref=ref, base=base):
            at = pl.multiple_of(i * 16, 16)
            to = pl.multiple_of(base + i * 16, 16)
            hid_ref[pl.ds(to, 16), :] = modulate(ref[pl.ds(at, 16), :].astype(F32), shift_row, scale_row)
            return carry

        lax.fori_loop(0, ROWS // 16, rows_at, 0)
    raw = dot_f32(hid_ref[...], ws_ref[...])
    pre_ref[:, :WD] = dot_f32(hid_ref[...], wv_ref[...]).astype(BF16)
    pre_ref[:, WD:] = dot_f32(hid_ref[...], ww_ref[...]).astype(BF16)

    raw_t = jnp.concatenate([raw[k * 128 : (k + 1) * 128].T[:16] for k in range(BLOCKS)], axis=1)
    pace = pace_ref[:, pl.ds(pl.multiple_of(sp * TOK, 128), TOK)]
    step = jax.nn.softplus(rounded(raw_t)) * pace
    decay = -rate_ref[:, 0:1] * step
    src = iota((BLOCK, BLOCK), 0)
    dst = iota((BLOCK, BLOCK), 1)
    up_to = (src <= dst).astype(F32)
    from_on = (src >= dst).astype(F32)
    is_forward = iota((16, BLOCK), 0) < HEADS_DEV
    cum = []
    tot = []
    for k in range(BLOCKS):
        part = decay[:, k * 128 : (k + 1) * 128]
        cum.append(jnp.where(is_forward, dot_exact(part, up_to), dot_exact(part, from_on)))
        tot.append(jnp.sum(part, axis=1, keepdims=True))
    zero = jnp.zeros((16, 1), F32)
    before = [sum(tot[:k], zero) for k in range(BLOCKS)]
    after = [sum(tot[k + 1 :], zero) for k in range(BLOCKS)]
    forward_col = iota((16, 1), 0) < HEADS_DEV
    for k in range(BLOCKS):
        st = step[:, k * 128 : (k + 1) * 128]
        to_end = jnp.where(forward_col, after[k], before[k])
        from_start = jnp.where(forward_col, before[k], after[k])
        rest = tot[k] - cum[k]
        stack = jnp.concatenate(
            [
                cum[k],
                jnp.exp(rest) * st,
                jnp.exp(cum[k]),
                jnp.exp(cum[k] + from_start),
                jnp.exp(rest + to_end) * st,
                jnp.zeros((48, BLOCK), F32),
            ],
            axis=0,
        )
        col_ref[k * 128 : (k + 1) * 128, :] = stack.T
        aux_ref[0:16, k * 128 : (k + 1) * 128] = cum[k]
        aux_ref[16:32, k * 128 : (k + 1) * 128] = st
        dec_ref[k : k + 1, :] = jnp.exp(head_row(tot[k][0:HEADS_DEV]))
        dec_ref[BLOCKS + k : BLOCKS + k + 1, :] = jnp.exp(head_row(tot[k][HEADS_DEV:]))
    whole = sum(tot, zero)

    shifts = block_shifts()
    vcol = pl.multiple_of(y * WD, 128)
    wcol = pl.multiple_of(y * KD, 128)
    taps = jnp.concatenate([vt_ref[:, pl.ds(vcol, WD)], wt_ref[:, pl.ds(wcol, KD)]], axis=1)

    def block_at(k, carry):
        rows = pl.ds(pl.multiple_of(k * BLOCK, BLOCK), BLOCK)
        for c in range(3):
            at = slice(c * 256, (c + 1) * 256)
            done = convolved(pre_ref[rows, at], shifts, taps[:, at])
            if c < 2:
                val_ref[rows, at] = done
            else:
                wri_ref[rows, :] = done
        cols = col_ref[rows, :]
        values = val_ref[rows, :].astype(F32)
        svf_ref[rows, :] = (values * head_lanes(cols, 64)).astype(BF16)
        svb_ref[rows, :] = (values * head_lanes(cols, 72)).astype(BF16)
        return carry

    lax.fori_loop(0, BLOCKS, block_at, 0)
    ends = [
        jnp.concatenate(
            [
                dot_tn(wri_ref[:, g * STATE : (g + 1) * STATE], ref[:, g * 256 : (g + 1) * 256])
                for g in range(GROUPS_DEV)
            ],
            axis=1,
        )
        for ref in (svf_ref, svb_ref)
    ]
    pack_states(scr, ends[0], ends[1], head_row(whole[0:HEADS_DEV]), head_row(whole[HEADS_DEV:]))
    send_order(scr, (o0, o1, o2, o3))


def second_body(
    hid_ref,
    val_ref,
    wri_ref,
    aux_ref,
    col_ref,
    dec_ref,
    wg_ref,
    wr_ref,
    rt_ref,
    rea_ref,
    loc_ref,
    ef_ref,
    eb_ref,
    sg_ref,
    pre_ref,
):
    y = lax.axis_index("tp")
    sg_ref[...] = silu(rounded(dot_f32(hid_ref[...], wg_ref[...])))
    pre_ref[...] = dot_f32(hid_ref[...], wr_ref[...]).astype(BF16)
    shifts = block_shifts()
    taps = rt_ref[:, pl.ds(pl.multiple_of(y * KD, 128), KD)]
    src = iota((BLOCK, BLOCK), 1)
    dst = iota((BLOCK, BLOCK), 0)

    def inside(k, carry):
        start = pl.multiple_of(k * BLOCK, BLOCK)
        rows = pl.ds(start, BLOCK)
        reads = convolved(pre_ref[rows, :], shifts, taps)
        rea_ref[rows, :] = reads
        cols = col_ref[rows, :]
        aux = aux_ref[:, rows]
        values = val_ref[rows, :]
        for g in range(GROUPS_DEV):
            states = slice(g * STATE, (g + 1) * STATE)
            affinity = dot_nt(reads[:, states], wri_ref[rows, states])
            for pair in range(2):
                outs = []
                for h in (4 * g + 2 * pair, 4 * g + 2 * pair + 1):
                    b = HEADS_DEV + h
                    exponent = jnp.where(
                        src <= dst, cols[:, h : h + 1] - aux[h : h + 1, :], cols[:, b : b + 1] - aux[b : b + 1, :]
                    )
                    fstep = aux[16 + h : 17 + h, :]
                    bstep = aux[16 + b : 17 + b, :]
                    weight = jnp.where(src < dst, fstep, jnp.where(src > dst, bstep, fstep + bstep))
                    mixing = (affinity * jnp.exp(exponent) * weight).astype(BF16)
                    outs.append(dot_f32(mixing, values[:, h * HEAD : (h + 1) * HEAD]))
                first = (4 * g + 2 * pair) * HEAD
                loc_ref[rows, first : first + 128] = jnp.concatenate(outs, axis=1)
        ef_ref[rows, :] = head_lanes(cols, 48)
        eb_ref[rows, :] = head_lanes(cols, 56)
        return carry

    lax.fori_loop(0, BLOCKS, inside, 0)

    for base, order, dec_at in ((0, (0, 1, 2, 3), 0), (HEADS_DEV, (3, 2, 1, 0), BLOCKS)):
        state = None
        for at, k in enumerate(order):
            rows = slice(k * BLOCK, (k + 1) * BLOCK)
            if state is not None:
                grown = head_lanes(col_ref[rows, :], 32 + base)
                for g in range(GROUPS_DEV):
                    lanes = slice(g * 256, (g + 1) * 256)
                    carried = dot_f32(rea_ref[rows, g * STATE : (g + 1) * STATE], state[:, lanes].astype(BF16))
                    loc_ref[rows, lanes] = loc_ref[rows, lanes] + carried * grown[:, lanes]
            if at < BLOCKS - 1:
                scaled = (val_ref[rows, :].astype(F32) * head_lanes(col_ref[rows, :], 16 + base)).astype(BF16)
                gain = jnp.concatenate(
                    [
                        dot_tn(wri_ref[rows, g * STATE : (g + 1) * STATE], scaled[:, g * 256 : (g + 1) * 256])
                        for g in range(GROUPS_DEV)
                    ],
                    axis=1,
                )
                state = gain if state is None else dec_ref[dec_at + k : dec_at + k + 1, :] * state + gain


def row_order(refs, order):
    x = lax.axis_index("sp_1")
    for d, ref in enumerate(refs):
        order[lax.rem(x - d + NX, NX)] = ref[...]


def row_step(order, i, state, backward):
    msg = order.at[i]
    decay = joined_row(msg, 2 * STATE)[1 if backward else 0]
    part = msg[STATE : 2 * STATE, :] if backward else msg[0:STATE, :]
    return jnp.exp(decay) * state + part.astype(F32)


def row_decay(order, backward):
    return sum(joined_row(order.at[i], 2 * STATE)[1 if backward else 0] for i in range(NX))


def across(order, state, backward):
    for i in reversed(range(NX)) if backward else range(NX):
        state = row_step(order, i, state, backward)
    return state


def ctx_row_body(m0, m1, m2, m3, f_ref, b_ref, low_ref, high_ref, order):
    z = lax.axis_index("sp_0")
    row_order((m0, m1, m2, m3), order)
    empty = jnp.zeros((STATE, 128), F32)
    for ref, backward in ((f_ref, False), (b_ref, True)):
        ref[0:STATE, :] = across(order, empty, backward).astype(BF16)
        ref[STATE:, :] = split_rows(row_decay(order, backward))
    near = z < NZ // 2
    low_ref[...] = jnp.where(near, f_ref[...].astype(F32), b_ref[...].astype(F32)).astype(BF16)
    high_ref[...] = jnp.where(near, b_ref[...].astype(F32), f_ref[...].astype(F32)).astype(BF16)


def latent_row_body(*refs):
    m = refs[0:4]
    cf_ref, cb_ref = refs[4:6]
    c = refs[6:13]
    outs = refs[13:20]
    ctx_out, order = refs[20:22]
    z = lax.axis_index("sp_0")
    row_order(m, order)
    first = z == 0
    last = z == NZ - 1
    ctx = jnp.where(first, cf_ref[0:STATE, :].astype(F32), cb_ref[0:STATE, :].astype(F32))
    for d in range(1, NZ):
        decay = joined_row(c[d - 1], STATE)[0]
        ctx = jnp.exp(decay) * ctx + c[d - 1][0:STATE, :].astype(F32)
    ctx_out[...] = ctx
    forward = across(order, jnp.where(first, ctx, 0.0), False)
    backward = across(order, jnp.where(last, ctx, 0.0), True)
    forward_rows = split_rows(row_decay(order, False)).astype(F32)
    backward_rows = split_rows(row_decay(order, True)).astype(F32)
    for d in range(1, NZ):
        ahead = z + d < NZ
        outs[d - 1][0:STATE, :] = jnp.where(ahead, forward, backward).astype(BF16)
        outs[d - 1][STATE:, :] = jnp.where(ahead, forward_rows, backward_rows).astype(BF16)


def start_body(*refs):
    m = refs[0:4]
    ctx_ref = refs[4]
    t = refs[5:12]
    outs = refs[12:16]
    order, scr = refs[16:18]
    z = lax.axis_index("sp_0")
    row_order(m, order)
    ctx = ctx_ref[...]
    forward = jnp.where(z == 0, ctx, 0.0)
    backward = jnp.where(z == NZ - 1, ctx, 0.0)
    for d in reversed(range(1, NZ)):
        decay = joined_row(t[d - 1], STATE)[0]
        forward = jnp.where(d <= z, jnp.exp(decay) * forward + t[d - 1][0:STATE, :].astype(F32), forward)
    for d in range(1, NZ):
        decay = joined_row(t[d - 1], STATE)[0]
        backward = jnp.where(d > z, jnp.exp(decay) * backward + t[d - 1][0:STATE, :].astype(F32), backward)
    for i in range(NX):
        scr[i, 0:STATE, :] = forward.astype(BF16)
        if i < NX - 1:
            forward = row_step(order, i, forward, False)
    for i in reversed(range(NX)):
        scr[i, STATE : 2 * STATE, :] = backward.astype(BF16)
        if i > 0:
            backward = row_step(order, i, backward, True)
    send_order(scr, outs)


def last_body(
    s0, s1, s2, s3, rea_ref, loc_ref, ef_ref, eb_ref, sg_ref, gain_ref, wo_ref, o0, o1, o2, o3, start, inner
):
    x = lax.axis_index("sp_1")
    y = lax.axis_index("tp")
    for d, ref in enumerate((s0, s1, s2, s3)):
        start[lax.rem(x - d + NX, NX)] = ref[...]
    gain = gain_ref[:, pl.ds(pl.multiple_of(y * WD, 128), WD)]
    for d in range(NY):
        rows = pl.ds(pl.multiple_of(lax.rem(y + d, NY) * ROWS, ROWS), ROWS)
        for g in range(GROUPS_DEV):
            lanes = slice(g * 256, (g + 1) * 256)
            reads = rea_ref[rows, g * STATE : (g + 1) * STATE]
            total = loc_ref[rows, lanes]
            for first, grown in ((0, ef_ref), (STATE, eb_ref)):
                state = jnp.concatenate(
                    [start[2 * g, first : first + STATE, :], start[2 * g + 1, first : first + STATE, :]], axis=1
                )
                total = total + dot_f32(reads, state) * grown[rows, lanes]
            gated = total * sg_ref[rows, lanes]
            scale = lax.rsqrt(jnp.mean(gated * gated, -1, keepdims=True) + GATED_FLOOR)
            inner[d * ROWS : (d + 1) * ROWS, lanes] = (gated * scale * gain[:, lanes]).astype(BF16)
    for d, ref in enumerate((o0, o1, o2, o3)):
        ref[...] = dot_f32(inner[d * ROWS : (d + 1) * ROWS, :], wo_ref[...]).astype(BF16)


def turned(n, d):
    return [(i, (i + d) % n) for i in range(n)]


def summed_over(value, axis, n):
    arrived = [lax.ppermute(value, axis, turned(n, d)) for d in range(1, n)]
    return sum(arrived, value)


def per_device(
    latent,
    condition,
    context,
    context_cond,
    shift_matrix,
    scale_matrix,
    gate_matrix,
    value_proj,
    gate_proj,
    write_proj,
    read_proj,
    step_proj,
    decay_rate,
    pacing,
    value_taps,
    write_taps,
    read_taps,
    norm_gain,
    out_proj,
):
    y = lax.axis_index("tp")
    own = latent[0]
    near = [lax.ppermute(own, "tp", turned(NY, d)) for d in range(1, NY)]
    count = NZ * NX
    ctx = context[0]
    left = lax.ppermute(ctx[CTX_DEV - 8 :], SP, [(i, i + 1) for i in range(count - 1)])
    right = lax.ppermute(ctx[:8], SP, [(i + 1, i) for i in range(count - 1)])

    (mod,) = call(
        mod_body,
        [((80, 128), F32)],
        (condition, context_cond.reshape(1, D), shift_matrix, scale_matrix, gate_matrix),
        name="mod",
    )
    mod = summed_over(mod, "sp_1", NX)
    mod = summed_over(mod, "sp_0", NZ)
    mod = summed_over(mod, "tp", NY)

    step_cols = lax.dynamic_slice_in_dim(step_proj, y * HEADS_DEV, HEADS_DEV, 2).reshape(D, 2 * HEADS_DEV)
    step_cols = jnp.pad(step_cols, ((0, 0), (0, 128 - 2 * HEADS_DEV)))
    rates = lax.dynamic_slice_in_dim(decay_rate, y * HEADS_DEV, HEADS_DEV, 1).reshape(1, 2 * HEADS_DEV)
    rate_row = jnp.pad(rates, ((0, 0), (0, 128 - 2 * HEADS_DEV)))
    rate_col = jnp.broadcast_to(rates.reshape(2 * HEADS_DEV, 1), (2 * HEADS_DEV, 128))

    msg = [((MSG, 128), BF16)] * 4
    msg_scr = pltpu.VMEM((NX, MSG, 128), BF16)
    ctx_out = call(
        ctx_body,
        msg,
        (ctx, left, right, mod, value_proj, write_proj, step_cols, rate_row, value_taps, write_taps),
        scratch=(msg_scr,),
        flops=150000000,
        name="ctx",
    )
    ctx_row = [ctx_out[0]] + [lax.ppermute(ctx_out[d], "sp_1", turned(NX, d)) for d in range(1, NX)]

    first = call(
        first_body,
        [
            ((TOK, D), BF16),
            ((TOK, WD), BF16),
            ((TOK, KD), BF16),
            ((32, TOK), F32),
            ((TOK, 128), F32),
            ((2 * BLOCKS, WD), F32),
        ]
        + msg,
        (own, *near, mod, value_proj, write_proj, step_cols, rate_col, pacing, value_taps, write_taps),
        scratch=(
            pltpu.VMEM((TOK, WD + KD), BF16),
            pltpu.VMEM((TOK, WD), BF16),
            pltpu.VMEM((TOK, WD), BF16),
            msg_scr,
        ),
        flops=2000000000,
        name="first",
    )
    hidden, values, writes, aux, cols, decs = first[:6]
    row = [first[6]] + [lax.ppermute(first[6 + d], "sp_1", turned(NX, d)) for d in range(1, NX)]

    ctx_f, ctx_b, ctx_low, ctx_high = call(
        ctx_row_body,
        [((ZMSG, 128), BF16)] * 4,
        ctx_row,
        scratch=(msg_scr,),
        name="ctx_row",
    )
    ctx_far = [
        lax.ppermute(ctx_low if d < NZ // 2 else ctx_high, "sp_0", [(d, 0), (NZ - 1 - d, NZ - 1)])
        for d in range(1, NZ)
    ]

    row_out = call(
        latent_row_body,
        [((ZMSG, 128), BF16)] * (NZ - 1) + [((STATE, 128), F32)],
        (*row, ctx_f, ctx_b, *ctx_far),
        scratch=(msg_scr,),
        name="latent_row",
    )
    far = [lax.ppermute(row_out[d - 1], "sp_0", turned(NZ, d)) for d in range(1, NZ)]

    reads, local, grown_f, grown_b, gate = call(
        second_body,
        [((TOK, KD), BF16)] + [((TOK, WD), F32)] * 4,
        (hidden, values, writes, aux, cols, decs, gate_proj, read_proj, read_taps),
        scratch=(pltpu.VMEM((TOK, KD), BF16),),
        flops=4000000000,
        name="second",
    )

    starts = call(
        start_body,
        [((2 * STATE, 128), BF16)] * 4,
        (*row, row_out[NZ - 1], *far),
        scratch=(msg_scr, pltpu.VMEM((NX, 2 * STATE, 128), BF16)),
        name="start",
    )
    start = [starts[0]] + [lax.ppermute(starts[d], "sp_1", turned(NX, d)) for d in range(1, NX)]

    outs = call(
        last_body,
        [((ROWS, D), BF16)] * 4,
        (*start, reads, local, grown_f, grown_b, gate, norm_gain.reshape(1, D), out_proj),
        scratch=(pltpu.VMEM((NX, 2 * STATE, 128), BF16), pltpu.VMEM((TOK, WD), BF16)),
        flops=1500000000,
        name="last",
    )
    parts = [outs[0]] + [lax.ppermute(outs[d], "tp", turned(NY, d)) for d in range(1, NY)]
    total = sum((p.astype(F32) for p in parts[1:]), parts[0].astype(F32))
    mixed = lax.optimization_barrier(total.astype(BF16))
    gate_row = mod[64:80].reshape(1, D)
    updated = own.astype(F32) + gate_row * mixed.astype(F32)
    return updated.astype(BF16)[None]


def solution(mesh):
    torus = Mesh(
        mesh.devices.reshape(NZ, NX, mesh.shape["tp"], mesh.shape["dp"]), ("sp_0", "sp_1", "tp", "dp")
    )
    placed = (
        P("dp", SP_TP, None),
        P("dp", None),
        P("dp", SP, None),
        P(),
        P(SP_TP, None),
        P(SP_TP, None),
        P(SP_TP, None),
        P(None, "tp"),
        P(None, "tp"),
        P(None, "tp"),
        P(None, "tp"),
        P(),
        P(),
        P("dp", None),
        P(),
        P(),
        P(),
        P(),
        P("tp", None),
    )
    return jax.shard_map(
        per_device, mesh=torus, in_specs=placed, out_specs=P("dp", SP_TP, None), check_vma=False
    )
```
